32 devices in a mesh: ep: 16 (over z, y, x), tp: 2 (over core).
Axes of the slice: x: 2, y: 2, z: 4, core: 2. Of those that a mesh axis runs over, the one named last changes fastest.
Arguments:
- tokens: bfloat16 [256, 2048], P('ep'), may hold values from -6 to 6
- recurrent_state: float32 [256, 4, 128, 256], P('ep', 'tp'), may hold values from -6 to 6
- query_weight: bfloat16 [2048, 512], P(None, 'tp'), may hold values from -0.125 to 0.125
- key_weight: bfloat16 [2048, 512], P(None, 'tp'), may hold values from -0.125 to 0.125
- decay_weight: bfloat16 [2048, 512], P(None, 'tp'), may hold values from -0.5 to 0.5
- value_weight: bfloat16 [2048, 1024], P(None, 'tp'), may hold values from -0.125 to 0.125
- gate_weight: bfloat16 [2048, 1024], P(None, 'tp'), may hold values from -0.125 to 0.125
- head_gain: float32 [256], replicated, may hold values from 0.1 to 1.9
- output_weight: bfloat16 [1024, 2048], P('tp'), may hold values from -0.375 to 0.375
- norm_gain: float32 [2, 2048], replicated, may hold values from 0.1 to 1.9
- norm_bias: float32 [2, 2048], replicated, may hold values from -1.8 to 1.8
- group_router: bfloat16 [2048, 4], replicated, may hold values from -0.125 to 0.125
- router_weight: bfloat16 [2048, 32], replicated, may hold values from -0.125 to 0.125
- routes: int32 [256, 2], P('ep'), may hold values from 0 to 31, as said below
- expert_gate: bfloat16 [32, 2048, 256], P(('ep', 'tp')), may hold values from -0.125 to 0.125
- expert_up: bfloat16 [32, 2048, 256], P(('ep', 'tp')), may hold values from -0.125 to 0.125
- expert_down: bfloat16 [32, 256, 2048], P(('ep', 'tp')), may hold values from -1.5 to 1.5
Outputs:
- new_tokens: bfloat16 [256, 2048], P('ep', 'tp')
- new_state: float32 [256, 4, 128, 256], P('ep', 'tp')
The draws below stay inside these ranges and needn't reach their ends.
Inputs may be any that keep to these rules, and one draw needn't show every extreme that they name: `routes`: each row names two different experts of one group (group g holds the experts g * 8 to g * 8 + 7). In the rows of one device each group is named by the same number of rows and no expert by more than 2 rows; some expert is named by exactly 2 rows of every device.
All inputs are finite; a program needn't handle non-finite values.
Results may differ from the reference program's by a relative error of at most 0.01.
Values may be sent and summed in bfloat16 or wider, within the bound.
A program may use at most 128 MiB of HBM per device.

```python
import jax
import jax.numpy as jnp
from jax import lax

D = 2048
HEADS = 4
DK = 128
DV = 256
EXPERT_FF = 256
GROUPS = 4
TOPK = 2
SEQ_DEV = 16
KW = 512
VW = 1024
EXPERTS = 32
EPG = 8
BATCH = 256
CAP = 2
N_EP = 16
N_TP = 2


def draw_routes(key, part):
    per_group = EXPERTS // GROUPS
    block_keys = jax.random.split(jax.random.fold_in(key, 11), N_EP)

    def permute(subkey):
        return jax.random.permutation(subkey, SEQ_DEV)
    rank_order = jax.vmap(permute)(block_keys).astype(jnp.int32)
    group_id = rank_order % GROUPS
    within_group = rank_order // GROUPS
    offsets = jax.random.randint(jax.random.fold_in(key, 12), (N_EP, GROUPS), 0, per_group).astype(jnp.int32)
    offsets = offsets.at[0, 0].set(0).at[0, GROUPS - 1].set(per_group - 1)
    extra_gap = jax.random.randint(jax.random.fold_in(key, 14), (N_EP, GROUPS), 0, 2).astype(jnp.int32)
    row_offset = jnp.take_along_axis(offsets, group_id, axis=1)
    row_gap = jnp.take_along_axis(extra_gap, group_id, axis=1)
    first_pick = group_id * per_group + (within_group + row_offset) % per_group
    second_pick = group_id * per_group + (within_group + row_offset + 1 + row_gap) % per_group
    flip_bits = jax.random.randint(jax.random.fold_in(key, 13), (N_EP, SEQ_DEV), 0, 2)
    lead_pick = jnp.where(flip_bits == 1, second_pick, first_pick)
    trail_pick = jnp.where(flip_bits == 1, first_pick, second_pick)
    return jnp.stack([lead_pick, trail_pick], axis=-1).reshape(BATCH, 2).astype(jnp.int32)


def level_of(own_key, extent, shards, smallest, largest):
    gain = 1.0
    for position, shards_of in shards:
        steps = jax.random.uniform(jax.random.fold_in(jax.random.fold_in(own_key, 6), position), (shards_of,), jnp.float32, smallest / len(shards), largest / len(shards))
        gain = gain * jnp.repeat(jnp.exp(steps), extent[position] // shards_of).reshape((-1,) + (1,) * (len(extent) - 1 - position))
    return gain


def centred(own_key, extent, width, bound, cuts=(), kind=jnp.bfloat16):
    array = width * jax.random.normal(own_key, extent, jnp.float32)
    if cuts:
        array = array * level_of(own_key, extent, cuts, -0.22, 0.18)
    return jnp.clip(array, -bound, bound).astype(kind)


def setup_inputs(seed: int = 0) -> dict:
    key_list = jax.random.split(jax.random.key(seed), 18)
    return {
        "tokens": centred(key_list[0], (BATCH, D), 1.0, 6.0, ((0, 16),)),
        "recurrent_state": centred(key_list[1], (BATCH, HEADS, DK, DV), 1.0, 6.0, ((0, 16), (1, 2)), jnp.float32),
        "query_weight": centred(key_list[2], (D, KW), D ** -0.5, 0.125, ((1, 2),)),
        "key_weight": centred(key_list[3], (D, KW), D ** -0.5, 0.125, ((1, 2),)),
        "decay_weight": centred(key_list[4], (D, KW), (D // 16) ** -0.5, 0.5, ((1, 2),)),
        "value_weight": centred(key_list[5], (D, VW), D ** -0.5, 0.125, ((1, 2),)),
        "gate_weight": centred(key_list[6], (D, VW), D ** -0.5, 0.125, ((1, 2),)),
        "head_gain": jnp.clip(1.0 + 0.18 * jax.random.normal(key_list[7], (DV,), jnp.float32), 0.1, 1.9),
        "output_weight": centred(key_list[8], (VW, D), (VW // 4) ** -0.5, 0.375, ((0, 2),)),
        "norm_gain": jnp.clip(1.0 + 0.18 * jax.random.normal(key_list[9], (2, D), jnp.float32), 0.1, 1.9),
        "norm_bias": centred(key_list[10], (2, D), 0.3, 1.8, (), jnp.float32),
        "group_router": centred(key_list[11], (D, GROUPS), D ** -0.5, 0.125),
        "router_weight": centred(key_list[12], (D, EXPERTS), D ** -0.5, 0.125),
        "routes": draw_routes(jax.random.fold_in(key_list[17], 71), 0),
        "expert_gate": centred(key_list[14], (EXPERTS, D, EXPERT_FF), D ** -0.5, 0.125, ((0, 32),)),
        "expert_up": centred(key_list[15], (EXPERTS, D, EXPERT_FF), D ** -0.5, 0.125, ((0, 32),)),
        "expert_down": centred(key_list[16], (EXPERTS, EXPERT_FF, D), (EXPERT_FF // 16) ** -0.5, 1.5, ((0, 32),)),
    }


alpha_res = 2.0 ** 0.5
eps_norm = 1e-05

def layer_normed(inputs, gain_row, bias_row):
    centered = inputs - lax.optimization_barrier(jnp.mean(inputs, axis=-1, keepdims=True))
    spread = lax.optimization_barrier(jnp.mean(centered * centered, axis=-1, keepdims=True))
    return centered * lax.rsqrt(spread + eps_norm) * gain_row + bias_row

def rounded_back(values_in):
    return lax.optimization_barrier(values_in.astype(jnp.bfloat16)).astype(jnp.float32)

def reference(tokens, recurrent_state, query_weight, key_weight, decay_weight, value_weight, gate_weight, head_gain, output_weight, norm_gain, norm_bias, group_router, router_weight, routes, expert_gate, expert_up, expert_down):

    def project(weight):
        return jnp.dot(tokens, weight, preferred_element_type=jnp.float32)
    queries = project(query_weight).reshape(BATCH, HEADS, DK) * DK ** (-0.5)
    key_rows = project(key_weight).reshape(BATCH, HEADS, DK)
    value_rows = project(value_weight).reshape(BATCH, HEADS, DV)
    gate_rows = project(gate_weight)
    log_decay = (jax.nn.log_sigmoid(project(decay_weight)) / 16.0).reshape(BATCH, HEADS, DK)
    new_state = jnp.exp(log_decay)[..., None] * recurrent_state + key_rows[..., None] * value_rows[:, :, None, :]
    readout = lax.optimization_barrier(jnp.sum(queries[..., None] * new_state, axis=2))
    norm_scale = lax.rsqrt(lax.optimization_barrier(jnp.mean(readout * readout, axis=-1, keepdims=True)) + eps_norm)
    gated = ((readout * norm_scale * head_gain).reshape(BATCH, VW) * jax.nn.silu(gate_rows)).astype(jnp.bfloat16)
    group_cols = VW // N_TP
    mixed_sum = jnp.zeros((BATCH, D), jnp.float32)
    for part_index in range(N_TP):
        product_part = jnp.dot(gated[:, part_index * group_cols:(part_index + 1) * group_cols], output_weight[part_index * group_cols:(part_index + 1) * group_cols], preferred_element_type=jnp.float32)
        mixed_sum = mixed_sum + rounded_back(product_part)
    hidden = layer_normed(alpha_res * tokens.astype(jnp.float32) + mixed_sum, norm_gain[0], norm_bias[0]).astype(jnp.bfloat16)
    group_logit = jnp.dot(hidden, group_router, preferred_element_type=jnp.float32)
    expert_logit = jnp.dot(hidden, router_weight, preferred_element_type=jnp.float32)
    chosen_group = routes[:, 0] // EPG
    group_hit = chosen_group[:, None] == jnp.arange(GROUPS, dtype=jnp.int32)[None, :]
    own_logit = lax.optimization_barrier(jnp.sum(jnp.where(group_hit, group_logit, 0.0), axis=1, keepdims=True))
    group_share = 1.0 / lax.optimization_barrier(jnp.sum(jnp.exp(group_logit - own_logit), axis=1))
    expert_hit = routes[:, :, None] == jnp.arange(EXPERTS, dtype=jnp.int32)[None, None, :]
    picked = lax.optimization_barrier(jnp.sum(jnp.where(expert_hit, expert_logit[:, None, :], 0.0), axis=2))
    route_weight = group_share[:, None] * jax.nn.sigmoid(picked - picked[:, ::-1])
    flat_routes = routes.reshape(BATCH * TOPK)
    row_limit = N_EP * CAP

    def serve_expert(expert_index):
        hit_index = jnp.nonzero(flat_routes == expert_index, size=row_limit, fill_value=BATCH * TOPK)[0].astype(jnp.int32)
        rows_in = hidden[jnp.minimum(hit_index, BATCH * TOPK - 1) // TOPK]
        gate_part = jnp.dot(rows_in, expert_gate[expert_index], preferred_element_type=jnp.float32)
        up_part = jnp.dot(rows_in, expert_up[expert_index], preferred_element_type=jnp.float32)
        activation = (jax.nn.silu(gate_part) * up_part).astype(jnp.bfloat16)
        combined = jnp.dot(activation, expert_down[expert_index], preferred_element_type=jnp.float32)
        return (hit_index, combined.astype(jnp.bfloat16))
    all_index, all_out = lax.map(serve_expert, jnp.arange(EXPERTS, dtype=jnp.int32))
    expert_out = jnp.zeros((BATCH * TOPK, D), jnp.bfloat16).at[all_index.reshape(-1)].set(all_out.reshape(-1, D), mode='drop')
    routed_sum = lax.optimization_barrier(jnp.sum(route_weight[..., None] * expert_out.reshape(BATCH, TOPK, D).astype(jnp.float32), axis=1))
    new_tokens = layer_normed(alpha_res * hidden.astype(jnp.float32) + routed_sum, norm_gain[1], norm_bias[1]).astype(jnp.bfloat16)
    return (new_tokens, new_state)
```

```python
import functools

import jax
import jax.numpy as jnp
from jax import lax
from jax.experimental import pallas as pl
from jax.experimental.pallas import tpu as pltpu
from jax.sharding import PartitionSpec as P

MESH = pl.DeviceIdType.MESH
alpha_res = 2.0**0.5
eps_norm = 1e-05
F32 = jnp.float32
BF16 = jnp.bfloat16


def dot32(a, b):
    return jnp.dot(a, b, preferred_element_type=F32)


def attention_kernel(
    chunk,
    tokens_hbm,
    state_hbm,
    wq_hbm,
    wk_hbm,
    wd_hbm,
    wv_hbm,
    wg_hbm,
    gain_hbm,
    new_hbm,
    gated_ref,
    tokens,
    state,
    fresh,
    wq,
    wk,
    wd,
    wv,
    wg,
    gain,
    readout,
    in_sem,
    state_sem,
    out_sem,
):
    rows, heads, key_dim, value_dim = state.shape
    chunks = rows // chunk
    small = [
        (tokens_hbm, tokens),
        (wk_hbm, wk),
        (wd_hbm, wd),
        (wq_hbm, wq),
        (wv_hbm, wv),
        (wg_hbm, wg),
        (gain_hbm, gain),
    ]
    copies = [
        pltpu.make_async_copy(src, dst, in_sem.at[n]) for n, (src, dst) in enumerate(small)
    ]
    ins = [
        pltpu.make_async_copy(
            state_hbm.at[pl.ds(n * chunk, chunk)], state.at[pl.ds(n * chunk, chunk)], state_sem.at[n]
        )
        for n in range(chunks)
    ]
    outs = [
        pltpu.make_async_copy(
            fresh.at[pl.ds(n * chunk, chunk)], new_hbm.at[pl.ds(n * chunk, chunk)], out_sem.at[n]
        )
        for n in range(chunks)
    ]
    for n in range(5):
        copies[n].start()
    for one in ins:
        one.start()
    copies[5].start()
    copies[6].start()

    copies[0].wait()
    x = tokens[...]
    copies[1].wait()
    keys = dot32(x, wk[...])
    copies[2].wait()
    pre = dot32(x, wd[...])
    decay = jnp.exp((jnp.minimum(pre, 0.0) - jnp.log1p(jnp.exp(-jnp.abs(pre)))) / 16.0)
    copies[3].wait()
    queries = dot32(x, wq[...]) * key_dim ** (-0.5)
    copies[4].wait()
    values = dot32(x, wv[...])
    columns = []
    for h in range(heads):
        part = slice(h * key_dim, (h + 1) * key_dim)
        pad = jnp.zeros((key_dim - 3 * rows, key_dim), F32)
        stacked = jnp.concatenate([keys[:, part], decay[:, part], queries[:, part], pad], axis=0)
        columns.append(stacked.T)
    for n in range(chunks):
        ins[n].wait()
        for b in range(n * chunk, (n + 1) * chunk):
            for h in range(heads):
                col = columns[h]
                v = values[b : b + 1, h * value_dim : (h + 1) * value_dim]
                new = (
                    col[:, rows + b : rows + b + 1] * state[b, h]
                    + col[:, b : b + 1] * v
                )
                fresh[b, h] = new
                readout[b : b + 1, h * value_dim : (h + 1) * value_dim] = jnp.sum(
                    col[:, 2 * rows + b : 2 * rows + b + 1] * new, axis=0, keepdims=True
                )
        outs[n].start()
    copies[5].wait()
    gate = dot32(x, wg[...])
    copies[6].wait()
    for h in range(heads):
        part = slice(h * value_dim, (h + 1) * value_dim)
        r = readout[:, part]
        scale = lax.rsqrt(jnp.mean(r * r, axis=-1, keepdims=True) + eps_norm)
        gated_ref[:, part] = (r * scale * gain[...] * jax.nn.silu(gate[:, part])).astype(BF16)
    for one in outs:
        one.wait()


def layer_kernel(
    n_ep,
    n_tp,
    group_count,
    cap,
    gated_hbm,
    wo_hbm,
    tokens_hbm,
    norm_gain_hbm,
    norm_bias_hbm,
    group_hbm,
    router_hbm,
    routes_hbm,
    eg_hbm,
    eu_hbm,
    ed_hbm,
    out_ref,
    gated,
    wo,
    tokens,
    norm_gain,
    norm_bias,
    group_w,
    router_w,
    routes,
    eg,
    eu,
    ed,
    part_mine,
    part_other,
    outgoing,
    arrived,
    results,
    returned,
    stat_mine,
    stat_other,
    in_sem,
    pair_sem,
    stat_sem,
    go_send,
    go_recv,
    back_send,
    back_recv,
):
    me = lax.axis_index("ep")
    core = lax.axis_index("tp")
    rows, width = tokens.shape
    half = width // n_tp
    experts = router_w.shape[1]
    per_group = experts // group_count
    slots = n_ep * cap
    pairs = [
        (gated_hbm, gated),
        (wo_hbm, wo),
        (tokens_hbm, tokens),
        (norm_gain_hbm, norm_gain),
        (norm_bias_hbm, norm_bias),
        (routes_hbm, routes),
        (group_hbm, group_w),
        (router_hbm, router_w),
        (eg_hbm, eg),
        (eu_hbm, eu),
        (ed_hbm, ed),
    ]
    loads = [
        pltpu.make_async_copy(src, dst, in_sem.at[n]) for n, (src, dst) in enumerate(pairs)
    ]
    barrier = pltpu.get_barrier_semaphore()
    for c in range(1, n_tp):
        pl.semaphore_signal(
            barrier, inc=1, device_id=(me, lax.rem(core + c, n_tp)), device_id_type=MESH
        )

    def greet(i, carry):
        there = lax.rem(me + i, n_ep)
        for c in range(n_tp):
            pl.semaphore_signal(barrier, inc=1, device_id=(there, c), device_id_type=MESH)
        return carry

    lax.fori_loop(1, n_ep, greet, 0)
    for one in loads:
        one.start()

    loads[0].wait()
    loads[1].wait()
    part_mine[...] = dot32(gated[...], wo[...]).astype(BF16)

    loads[5].wait()
    chosen = routes[...]
    first, second = chosen[:, 0:1], chosen[:, 1:2]
    below = (
        lax.broadcasted_iota(jnp.int32, (rows, rows), 1)
        < lax.broadcasted_iota(jnp.int32, (rows, rows), 0)
    ).astype(BF16)

    def slot_of(count, to_expert):
        column = lax.broadcasted_iota(jnp.int32, (rows, count), 1)
        expert = to_expert(lax.div(column, cap))
        place = lax.rem(column, cap).astype(F32)
        hit0, hit1 = first == expert, second == expert
        either = jnp.where(hit0, 1.0, jnp.where(hit1, 1.0, 0.0))
        earlier = dot32(below, either.astype(BF16))
        placed = jnp.where(earlier == place, 1.0, 0.0)
        return jnp.where(hit0, placed, 0.0), jnp.where(hit1, placed, 0.0)

    send0, send1 = slot_of(slots, lambda j: j * n_tp + core)
    pick_send = (send0 + send1).astype(BF16)
    back0, back1 = slot_of(slots * n_tp, lambda j: j)
    back0, back1 = back0.astype(BF16), back1.astype(BF16)

    pl.semaphore_wait(barrier, n_ep * n_tp - 1)
    swap = pltpu.make_async_remote_copy(
        src_ref=part_mine,
        dst_ref=part_other,
        send_sem=pair_sem.at[0],
        recv_sem=pair_sem.at[1],
        device_id=(me, 1 - core),
        device_id_type=MESH,
    )
    swap.start()
    for n in (2, 3, 4):
        loads[n].wait()
    base = alpha_res * tokens[...].astype(F32) + part_mine[...].astype(F32)
    swap.wait()
    mixed = base + part_other[...].astype(F32)
    centered = mixed - jnp.mean(mixed, axis=-1, keepdims=True)
    spread = jnp.mean(centered * centered, axis=-1, keepdims=True)
    hidden = (
        centered * lax.rsqrt(spread + eps_norm) * norm_gain[0:1, :] + norm_bias[0:1, :]
    ).astype(BF16)

    packed = lax.dot_general(
        pick_send, hidden, (((0,), (0,)), ((), ())), preferred_element_type=F32
    )
    outgoing[...] = packed.reshape(n_ep, cap, width).astype(BF16)

    def dispatch(i):
        there = lax.rem(me + i, n_ep)
        return pltpu.make_async_remote_copy(
            src_ref=outgoing.at[there],
            dst_ref=arrived.at[me],
            send_sem=go_send.at[i],
            recv_sem=go_recv.at[i],
            device_id=(there, core),
            device_id_type=MESH,
        )

    def go(i, carry):
        dispatch(i).start()
        return carry

    lax.fori_loop(1, n_ep, go, 0)
    arrived[me] = outgoing[me]

    loads[6].wait()
    loads[7].wait()
    group_logit = dot32(hidden, group_w[...])
    expert_logit = dot32(hidden, router_w[...])
    own_group = lax.div(first, per_group)
    group_hit = own_group == lax.broadcasted_iota(jnp.int32, group_logit.shape, 1)
    own_logit = jnp.sum(jnp.where(group_hit, group_logit, 0.0), axis=1, keepdims=True)
    share = 1.0 / jnp.sum(jnp.exp(group_logit - own_logit), axis=1, keepdims=True)
    expert_iota = lax.broadcasted_iota(jnp.int32, expert_logit.shape, 1)
    logit0 = jnp.sum(jnp.where(first == expert_iota, expert_logit, 0.0), axis=1, keepdims=True)
    logit1 = jnp.sum(jnp.where(second == expert_iota, expert_logit, 0.0), axis=1, keepdims=True)
    weight0 = share * jax.nn.sigmoid(logit0 - logit1)
    weight1 = share * jax.nn.sigmoid(logit1 - logit0)
    for n in (8, 9, 10):
        loads[n].wait()

    def landed(i, carry):
        dispatch(i).wait()
        return carry

    lax.fori_loop(1, n_ep, landed, 0)
    rows_in = arrived[...].astype(F32).reshape(slots, width).astype(BF16)
    gate_part = dot32(rows_in, eg[0])
    up_part = dot32(rows_in, eu[0])
    activation = (jax.nn.silu(gate_part) * up_part).astype(BF16)
    result = dot32(activation, ed[0]).reshape(n_ep, cap, width).astype(BF16)
    for c in range(n_tp):
        results[c] = result[:, :, c * half : (c + 1) * half]

    def send_back(i, c):
        there = lax.rem(me + i, n_ep)
        to = lax.rem(core + c, n_tp)
        return pltpu.make_async_remote_copy(
            src_ref=results.at[to, there],
            dst_ref=returned.at[me * n_tp + core],
            send_sem=back_send.at[c, i],
            recv_sem=back_recv.at[c, i],
            device_id=(there, to),
            device_id_type=MESH,
        )

    def back(i, carry):
        for c in range(n_tp):
            send_back(i, c).start()
        return carry

    lax.fori_loop(1, n_ep, back, 0)
    for c in range(1, n_tp):
        send_back(0, c).start()
    returned[me * n_tp + core] = results[core, me]
    mine = jnp.where(core == 0, hidden[:, :half].astype(F32), hidden[:, half:].astype(F32))
    base = alpha_res * mine
    gain = jnp.where(core == 0, norm_gain[1:2, :half], norm_gain[1:2, half:])
    shift = jnp.where(core == 0, norm_bias[1:2, :half], norm_bias[1:2, half:])

    def home(i, carry):
        for c in range(n_tp):
            send_back(i, c).wait()
        return carry

    lax.fori_loop(1, n_ep, home, 0)
    for c in range(1, n_tp):
        send_back(0, c).wait()
    fetched = returned[...].astype(F32).reshape(slots * n_tp, half).astype(BF16)
    blended = base + weight0 * dot32(back0, fetched) + weight1 * dot32(back1, fetched)
    total = jnp.sum(blended, axis=1, keepdims=True)
    squares = jnp.sum(blended * blended, axis=1, keepdims=True)
    lane = lax.broadcasted_iota(jnp.int32, stat_mine.shape, 1)
    stats = jnp.where(lane == 0, total, squares)
    stat_mine[...] = stats
    trade = pltpu.make_async_remote_copy(
        src_ref=stat_mine,
        dst_ref=stat_other,
        send_sem=stat_sem.at[0],
        recv_sem=stat_sem.at[1],
        device_id=(me, 1 - core),
        device_id_type=MESH,
    )
    trade.start()
    trade.wait()
    both = stats + stat_other[...]
    row_mean = both[:, 0:1] / width
    spread = both[:, 1:2] / width - row_mean * row_mean
    out_ref[...] = (
        (blended - row_mean) * lax.rsqrt(spread + eps_norm) * gain + shift
    ).astype(BF16)


def on_device(
    n_ep,
    n_tp,
    tokens,
    recurrent_state,
    query_weight,
    key_weight,
    decay_weight,
    value_weight,
    gate_weight,
    head_gain,
    output_weight,
    norm_gain,
    norm_bias,
    group_router,
    router_weight,
    routes,
    expert_gate,
    expert_up,
    expert_down,
):
    rows, width = tokens.shape
    heads, key_dim, value_dim = recurrent_state.shape[1:]
    anywhere = pl.BlockSpec(memory_space=pl.ANY)
    vmem = pl.BlockSpec(memory_space=pltpu.VMEM)
    chunk = 2
    chunks = rows // chunk
    dma = pltpu.SemaphoreType.DMA

    def like(a):
        return pltpu.VMEM(a.shape, a.dtype)

    gain_row = head_gain.reshape(1, value_dim)
    new_state, gated = pl.pallas_call(
        functools.partial(attention_kernel, chunk),
        out_shape=(
            jax.ShapeDtypeStruct(recurrent_state.shape, F32),
            jax.ShapeDtypeStruct((rows, heads * value_dim), BF16),
        ),
        in_specs=[anywhere] * 8,
        out_specs=(anywhere, vmem),
        scratch_shapes=[
            like(tokens),
            like(recurrent_state),
            like(recurrent_state),
            like(query_weight),
            like(key_weight),
            like(decay_weight),
            like(value_weight),
            like(gate_weight),
            like(gain_row),
            pltpu.VMEM((rows, heads * value_dim), F32),
            dma((7,)),
            dma((chunks,)),
            dma((chunks,)),
        ],
        compiler_params=pltpu.CompilerParams(vmem_limit_bytes=40 * 1024 * 1024),
        name="attention",
    )(
        tokens,
        recurrent_state,
        query_weight,
        key_weight,
        decay_weight,
        value_weight,
        gate_weight,
        gain_row,
    )
    experts = router_weight.shape[1]
    cap = 2 * max(1, rows // experts)
    half = width // n_tp
    operands = (
        gated,
        output_weight,
        tokens,
        norm_gain,
        norm_bias,
        group_router,
        router_weight,
        routes,
        expert_gate,
        expert_up,
        expert_down,
    )
    new_tokens = pl.pallas_call(
        functools.partial(layer_kernel, n_ep, n_tp, group_router.shape[1], cap),
        out_shape=jax.ShapeDtypeStruct((rows, half), BF16),
        in_specs=[anywhere] * len(operands),
        out_specs=vmem,
        scratch_shapes=[like(a) for a in operands]
        + [
            pltpu.VMEM((rows, width), BF16),
            pltpu.VMEM((rows, width), BF16),
            pltpu.VMEM((n_ep, cap, width), BF16),
            pltpu.VMEM((n_ep, cap, width), BF16),
            pltpu.VMEM((n_tp, n_ep, cap, half), BF16),
            pltpu.VMEM((n_ep * n_tp, cap, half), BF16),
            pltpu.VMEM((rows, 128), F32),
            pltpu.VMEM((rows, 128), F32),
            dma((len(operands),)),
            dma((2,)),
            dma((2,)),
            dma((n_ep,)),
            dma((n_ep,)),
            dma((n_tp, n_ep)),
            dma((n_tp, n_ep)),
        ],
        compiler_params=pltpu.CompilerParams(
            collective_id=0, has_side_effects=True, vmem_limit_bytes=40 * 1024 * 1024
        ),
        name="layer",
    )(*operands)
    return new_tokens, new_state


def solution(mesh):
    in_specs = (
        P("ep", None),
        P("ep", "tp", None, None),
        P(None, "tp"),
        P(None, "tp"),
        P(None, "tp"),
        P(None, "tp"),
        P(None, "tp"),
        P(),
        P("tp", None),
        P(),
        P(),
        P(),
        P(),
        P("ep", None),
        P(("ep", "tp"), None, None),
        P(("ep", "tp"), None, None),
        P(("ep", "tp"), None, None),
    )
    out_specs = (P("ep", "tp"), P("ep", "tp", None, None))
    return jax.shard_map(
        functools.partial(on_device, mesh.shape["ep"], mesh.shape["tp"]),
        mesh=mesh,
        in_specs=in_specs,
        out_specs=out_specs,
        check_vma=False,
    )
```

```python
import functools

import jax
import jax.numpy as jnp
from jax import lax
from jax.experimental import pallas as pl
from jax.experimental.pallas import tpu as pltpu
from jax.sharding import PartitionSpec as P

MESH = pl.DeviceIdType.MESH
alpha_res = 2.0**0.5
eps_norm = 1e-05
F32 = jnp.float32
BF16 = jnp.bfloat16


def dot32(a, b):
    return jnp.dot(a, b, preferred_element_type=F32)


def attention_kernel(
    chunk,
    tokens_hbm,
    state_hbm,
    wq_hbm,
    wk_hbm,
    wd_hbm,
    wv_hbm,
    wg_hbm,
    gain_hbm,
    new_hbm,
    gated_hbm,
    tokens,
    state,
    fresh,
    wq,
    wk,
    wd,
    wv,
    wg,
    gain,
    readout,
    gated_ref,
    in_sem,
    state_sem,
    out_sem,
    gated_sem,
):
    rows, heads, key_dim, value_dim = state.shape
    chunks = rows // chunk
    small = [
        (tokens_hbm, tokens),
        (wk_hbm, wk),
        (wd_hbm, wd),
        (wq_hbm, wq),
        (wv_hbm, wv),
        (wg_hbm, wg),
        (gain_hbm, gain),
    ]
    copies = [
        pltpu.make_async_copy(src, dst, in_sem.at[n]) for n, (src, dst) in enumerate(small)
    ]
    ins = [
        pltpu.make_async_copy(
            state_hbm.at[pl.ds(n * chunk, chunk)], state.at[pl.ds(n * chunk, chunk)], state_sem.at[n]
        )
        for n in range(chunks)
    ]
    outs = [
        pltpu.make_async_copy(
            fresh.at[pl.ds(n * chunk, chunk)], new_hbm.at[pl.ds(n * chunk, chunk)], out_sem.at[n]
        )
        for n in range(chunks)
    ]
    for n in range(5):
        copies[n].start()
    for one in ins:
        one.start()
    copies[5].start()
    copies[6].start()

    copies[0].wait()
    x = tokens[...]
    copies[1].wait()
    keys = dot32(x, wk[...])
    copies[2].wait()
    pre = dot32(x, wd[...])
    decay = jnp.exp((jnp.minimum(pre, 0.0) - jnp.log1p(jnp.exp(-jnp.abs(pre)))) / 16.0)
    copies[3].wait()
    queries = dot32(x, wq[...]) * key_dim ** (-0.5)
    copies[4].wait()
    values = dot32(x, wv[...])
    columns = []
    for h in range(heads):
        part = slice(h * key_dim, (h + 1) * key_dim)
        pad = jnp.zeros((key_dim - 3 * rows, key_dim), F32)
        stacked = jnp.concatenate([keys[:, part], decay[:, part], queries[:, part], pad], axis=0)
        columns.append(stacked.T)
    for n in range(chunks):
        ins[n].wait()
        for b in range(n * chunk, (n + 1) * chunk):
            for h in range(heads):
                col = columns[h]
                v = values[b : b + 1, h * value_dim : (h + 1) * value_dim]
                new = (
                    col[:, rows + b : rows + b + 1] * state[b, h]
                    + col[:, b : b + 1] * v
                )
                fresh[b, h] = new
                readout[b : b + 1, h * value_dim : (h + 1) * value_dim] = jnp.sum(
                    col[:, 2 * rows + b : 2 * rows + b + 1] * new, axis=0, keepdims=True
                )
        outs[n].start()
    copies[5].wait()
    gate = dot32(x, wg[...])
    copies[6].wait()
    for h in range(heads):
        part = slice(h * value_dim, (h + 1) * value_dim)
        r = readout[:, part]
        scale = lax.rsqrt(jnp.mean(r * r, axis=-1, keepdims=True) + eps_norm)
        gated_ref[:, part] = (r * scale * gain[...] * jax.nn.silu(gate[:, part])).astype(BF16)
    rounded = pltpu.make_async_copy(gated_ref, gated_hbm, gated_sem.at[0])
    rounded.start()
    for one in outs:
        one.wait()
    rounded.wait()


def layer_kernel(
    n_ep,
    n_tp,
    cap,
    gated_hbm,
    wo_hbm,
    tokens_hbm,
    norm_gain_hbm,
    norm_bias_hbm,
    group_w_hbm,
    router_w_hbm,
    routes_hbm,
    eg_hbm,
    eu_hbm,
    ed_hbm,
    out_ref,
    gated,
    wo,
    tokens,
    norm_gain,
    norm_bias,
    group_w,
    router_w,
    routes,
    eg,
    eu,
    ed,
    part_mine,
    part_other,
    outgoing,
    arrived,
    results,
    returned,
    stat_mine,
    stat_other,
    in_sem,
    pair_sem,
    stat_sem,
    go_send,
    go_recv,
    back_send,
    back_recv,
):
    me = lax.axis_index("ep")
    core = lax.axis_index("tp")
    rows, width = tokens.shape
    half = width // n_tp
    per_group = router_w.shape[0] // group_w.shape[0]
    slots = n_ep * cap
    operands = [
        (gated_hbm, gated),
        (wo_hbm, wo),
        (routes_hbm, routes),
        (tokens_hbm, tokens),
        (norm_gain_hbm, norm_gain),
        (norm_bias_hbm, norm_bias),
        (group_w_hbm, group_w),
        (router_w_hbm, router_w),
        (eg_hbm, eg),
        (eu_hbm, eu),
        (ed_hbm, ed),
    ]
    order = sorted(range(1, n_ep), key=lambda i: abs(2 * i - n_ep))

    def over_peers(body):
        if n_ep <= 32:
            for i in order:
                body(i)
        else:

            def step(i, carry):
                body(i)
                return carry

            lax.fori_loop(1, n_ep, step, 0)

    barrier = pltpu.get_barrier_semaphore()

    def greet(i):
        for c in range(n_tp):
            pl.semaphore_signal(
                barrier, inc=1, device_id=(lax.rem(me + i, n_ep), c), device_id_type=MESH
            )

    loads = [
        pltpu.make_async_copy(src, dst, in_sem.at[n]) for n, (src, dst) in enumerate(operands)
    ]
    for one in loads:
        one.start()
    over_peers(greet)
    for c in range(1, n_tp):
        pl.semaphore_signal(
            barrier, inc=1, device_id=(me, lax.rem(core + c, n_tp)), device_id_type=MESH
        )

    loads[0].wait()
    loads[1].wait()
    part_mine[...] = dot32(gated[...], wo[...]).astype(BF16)

    loads[2].wait()
    first, second = routes[0:1, :], routes[1:2, :]
    before = (
        lax.broadcasted_iota(jnp.int32, (rows, rows), 0)
        < lax.broadcasted_iota(jnp.int32, (rows, rows), 1)
    ).astype(BF16)

    def slot_of(count, to_expert):
        line = lax.broadcasted_iota(jnp.int32, (count, rows), 0)
        expert = to_expert(lax.div(line, cap))
        place = lax.rem(line, cap).astype(F32)
        hit0, hit1 = first == expert, second == expert
        either = jnp.where(hit0, 1.0, jnp.where(hit1, 1.0, 0.0))
        earlier = dot32(either.astype(BF16), before)
        placed = jnp.where(earlier == place, 1.0, 0.0)
        return jnp.where(hit0, placed, 0.0), jnp.where(hit1, placed, 0.0)

    send0, send1 = slot_of(slots, lambda j: j * n_tp + core)
    pick_send = (send0 + send1).astype(BF16)
    back0, back1 = slot_of(slots * n_tp, lambda j: j)
    for n in range(3, len(loads)):
        loads[n].wait()
    base = alpha_res * tokens[...].astype(F32) + part_mine[...].astype(F32)

    pl.semaphore_wait(barrier, n_ep * n_tp - 1)
    swap = pltpu.make_async_remote_copy(
        src_ref=part_mine,
        dst_ref=part_other,
        send_sem=pair_sem.at[0],
        recv_sem=pair_sem.at[1],
        device_id=(me, 1 - core),
        device_id_type=MESH,
    )
    swap.start()
    swap.wait()
    mixed = base + part_other[...].astype(F32)
    centered = mixed - jnp.mean(mixed, axis=-1, keepdims=True)
    spread = jnp.mean(centered * centered, axis=-1, keepdims=True)
    hidden = (
        centered * lax.rsqrt(spread + eps_norm) * norm_gain[0:1, :] + norm_bias[0:1, :]
    ).astype(BF16)

    outgoing[...] = dot32(pick_send, hidden).reshape(n_ep, cap, width).astype(BF16)

    def dispatch(i):
        there = lax.rem(me + i, n_ep)
        return pltpu.make_async_remote_copy(
            src_ref=outgoing.at[there],
            dst_ref=arrived.at[me],
            send_sem=go_send.at[i],
            recv_sem=go_recv.at[i],
            device_id=(there, core),
            device_id_type=MESH,
        )

    over_peers(lambda i: dispatch(i).start())
    arrived[me] = outgoing[me]

    across = (((1,), (1,)), ((), ()))
    group_logit = lax.dot_general(group_w[...], hidden, across, preferred_element_type=F32)
    expert_logit = lax.dot_general(router_w[...], hidden, across, preferred_element_type=F32)
    own_group = lax.div(first, per_group)
    group_hit = own_group == lax.broadcasted_iota(jnp.int32, group_logit.shape, 0)
    own_logit = jnp.sum(jnp.where(group_hit, group_logit, 0.0), axis=0, keepdims=True)
    share = 1.0 / jnp.sum(jnp.exp(group_logit - own_logit), axis=0, keepdims=True)
    expert_iota = lax.broadcasted_iota(jnp.int32, expert_logit.shape, 0)
    logit0 = jnp.sum(jnp.where(first == expert_iota, expert_logit, 0.0), axis=0, keepdims=True)
    logit1 = jnp.sum(jnp.where(second == expert_iota, expert_logit, 0.0), axis=0, keepdims=True)
    weighted = back0 * (share * jax.nn.sigmoid(logit0 - logit1)) + back1 * (
        share * jax.nn.sigmoid(logit1 - logit0)
    )
    upper = weighted.astype(BF16)
    lower = (weighted - upper.astype(F32)).astype(BF16)
    mine = jnp.where(core == 0, hidden[:, :half].astype(F32), hidden[:, half:].astype(F32))
    base = alpha_res * mine
    gain = jnp.where(core == 0, norm_gain[1:2, :half], norm_gain[1:2, half:])
    shift = jnp.where(core == 0, norm_bias[1:2, :half], norm_bias[1:2, half:])

    over_peers(lambda i: dispatch(i).wait())
    rows_in = arrived[...].astype(F32).reshape(slots, width).astype(BF16)
    gate_part = dot32(rows_in, eg[0])
    up_part = dot32(rows_in, eu[0])
    activation = (jax.nn.silu(gate_part) * up_part).astype(BF16)

    def send_back(i, c):
        there = lax.rem(me + i, n_ep)
        to = lax.rem(core + c, n_tp)
        return pltpu.make_async_remote_copy(
            src_ref=results.at[c, there],
            dst_ref=returned.at[me * n_tp + core],
            send_sem=back_send.at[c, i],
            recv_sem=back_recv.at[c, i],
            device_id=(there, to),
            device_id_type=MESH,
        )

    for c in range(n_tp):
        start = pl.multiple_of(lax.rem(core + c, n_tp) * half, half)
        result = dot32(activation, ed[0, :, pl.ds(start, half)])
        results[c] = result.reshape(n_ep, cap, half).astype(BF16)
        over_peers(lambda i: send_back(i, c).start())
        if c:
            send_back(0, c).start()
    returned[me * n_tp + core] = results[0, me]

    def home(i):
        for c in range(n_tp):
            send_back(i, c).wait()

    over_peers(home)
    for c in range(1, n_tp):
        send_back(0, c).wait()
    fetched = returned[...].astype(F32).reshape(slots * n_tp, half).astype(BF16)
    down = (((0,), (0,)), ((), ()))
    blended = (
        base
        + lax.dot_general(upper, fetched, down, preferred_element_type=F32)
        + lax.dot_general(lower, fetched, down, preferred_element_type=F32)
    )
    total = jnp.sum(blended, axis=1, keepdims=True)
    squares = jnp.sum(blended * blended, axis=1, keepdims=True)
    lane = lax.broadcasted_iota(jnp.int32, stat_mine.shape, 1)
    stats = jnp.where(lane == 0, total, squares)
    stat_mine[...] = stats
    trade = pltpu.make_async_remote_copy(
        src_ref=stat_mine,
        dst_ref=stat_other,
        send_sem=stat_sem.at[0],
        recv_sem=stat_sem.at[1],
        device_id=(me, 1 - core),
        device_id_type=MESH,
    )
    trade.start()
    trade.wait()
    both = stats + stat_other[...]
    row_mean = both[:, 0:1] / width
    spread = both[:, 1:2] / width - row_mean * row_mean
    out_ref[...] = (
        (blended - row_mean) * lax.rsqrt(spread + eps_norm) * gain + shift
    ).astype(BF16)


def on_device(
    n_ep,
    n_tp,
    tokens,
    recurrent_state,
    query_weight,
    key_weight,
    decay_weight,
    value_weight,
    gate_weight,
    head_gain,
    output_weight,
    norm_gain,
    norm_bias,
    group_router,
    router_weight,
    routes,
    expert_gate,
    expert_up,
    expert_down,
):
    rows, width = tokens.shape
    heads, key_dim, value_dim = recurrent_state.shape[1:]
    in_hbm = pl.BlockSpec(memory_space=pltpu.HBM)
    vmem = pl.BlockSpec(memory_space=pltpu.VMEM)
    chunk = 2
    chunks = rows // chunk
    dma = pltpu.SemaphoreType.DMA

    def like(a):
        return pltpu.VMEM(a.shape, a.dtype)

    gain_row = head_gain.reshape(1, value_dim)
    new_state, gated = pl.pallas_call(
        functools.partial(attention_kernel, chunk),
        out_shape=(
            jax.ShapeDtypeStruct(recurrent_state.shape, F32),
            jax.ShapeDtypeStruct((rows, heads * value_dim), BF16),
        ),
        in_specs=[in_hbm] * 8,
        out_specs=(in_hbm, in_hbm),
        scratch_shapes=[
            like(tokens),
            like(recurrent_state),
            like(recurrent_state),
            like(query_weight),
            like(key_weight),
            like(decay_weight),
            like(value_weight),
            like(gate_weight),
            like(gain_row),
            pltpu.VMEM((rows, heads * value_dim), F32),
            pltpu.VMEM((rows, heads * value_dim), BF16),
            dma((7,)),
            dma((chunks,)),
            dma((chunks,)),
            dma((1,)),
        ],
        compiler_params=pltpu.CompilerParams(vmem_limit_bytes=67043328),
        name="attention",
    )(
        tokens,
        recurrent_state,
        query_weight,
        key_weight,
        decay_weight,
        value_weight,
        gate_weight,
        gain_row,
    )
    experts = router_weight.shape[1]
    cap = 2 * max(1, rows // experts)
    half = width // n_tp
    operands = (
        gated,
        output_weight,
        tokens,
        norm_gain,
        norm_bias,
        group_router.T,
        router_weight.T,
        routes.T,
        expert_gate,
        expert_up,
        expert_down,
    )
    new_tokens = pl.pallas_call(
        functools.partial(layer_kernel, n_ep, n_tp, cap),
        out_shape=jax.ShapeDtypeStruct((rows, half), BF16),
        in_specs=[in_hbm] * len(operands),
        out_specs=vmem,
        scratch_shapes=[like(a) for a in operands]
        + [
            pltpu.VMEM((rows, width), BF16),
            pltpu.VMEM((rows, width), BF16),
            pltpu.VMEM((n_ep, cap, width), BF16),
            pltpu.VMEM((n_ep, cap, width), BF16),
            pltpu.VMEM((n_tp, n_ep, cap, half), BF16),
            pltpu.VMEM((n_ep * n_tp, cap, half), BF16),
            pltpu.VMEM((rows, 128), F32),
            pltpu.VMEM((rows, 128), F32),
            dma((len(operands),)),
            dma((2,)),
            dma((2,)),
            dma((n_ep,)),
            dma((n_ep,)),
            dma((n_tp, n_ep)),
            dma((n_tp, n_ep)),
        ],
        compiler_params=pltpu.CompilerParams(
            collective_id=0, has_side_effects=True, vmem_limit_bytes=67043328
        ),
        name="layer",
    )(*operands)
    return new_tokens, new_state


def solution(mesh):
    in_specs = (
        P("ep", None),
        P("ep", "tp", None, None),
        P(None, "tp"),
        P(None, "tp"),
        P(None, "tp"),
        P(None, "tp"),
        P(None, "tp"),
        P(),
        P("tp", None),
        P(),
        P(),
        P(),
        P(),
        P("ep", None),
        P(("ep", "tp"), None, None),
        P(("ep", "tp"), None, None),
        P(("ep", "tp"), None, None),
    )
    out_specs = (P("ep", "tp"), P("ep", "tp", None, None))
    return jax.shard_map(
        functools.partial(on_device, mesh.shape["ep"], mesh.shape["tp"]),
        mesh=mesh,
        in_specs=in_specs,
        out_specs=out_specs,
        check_vma=False,
    )
```

```python
import functools

import jax
import jax.numpy as jnp
from jax import lax
from jax.experimental import pallas as pl
from jax.experimental.pallas import tpu as pltpu
from jax.sharding import PartitionSpec as P

MESH = pl.DeviceIdType.MESH
alpha_res = 2.0**0.5
eps_norm = 1e-05
F32 = jnp.float32
BF16 = jnp.bfloat16


def dot32(a, b):
    return jnp.dot(a, b, preferred_element_type=F32)


def attention_kernel(
    chunk,
    tokens_hbm,
    state_hbm,
    wq_hbm,
    wk_hbm,
    wd_hbm,
    wv_hbm,
    gain_hbm,
    new_hbm,
    normed_hbm,
    tokens,
    state,
    fresh,
    wq,
    wk,
    wd,
    wv,
    gain,
    readout,
    normed,
    in_sem,
    state_sem,
    out_sem,
    normed_sem,
):
    rows, heads, key_dim, value_dim = state.shape
    chunks = rows // chunk
    small = [
        (tokens_hbm, tokens),
        (wk_hbm, wk),
        (wd_hbm, wd),
        (wq_hbm, wq),
        (wv_hbm, wv),
        (gain_hbm, gain),
    ]
    copies = [
        pltpu.make_async_copy(src, dst, in_sem.at[n]) for n, (src, dst) in enumerate(small)
    ]
    ins = [
        pltpu.make_async_copy(
            state_hbm.at[pl.ds(n * chunk, chunk)], state.at[pl.ds(n * chunk, chunk)], state_sem.at[n]
        )
        for n in range(chunks)
    ]
    outs = [
        pltpu.make_async_copy(
            fresh.at[pl.ds(n * chunk, chunk)], new_hbm.at[pl.ds(n * chunk, chunk)], out_sem.at[n]
        )
        for n in range(chunks)
    ]
    for n in range(5):
        copies[n].start()
    for one in ins:
        one.start()
    copies[5].start()

    copies[0].wait()
    x = tokens[...]
    copies[1].wait()
    keys = dot32(x, wk[...])
    copies[2].wait()
    pre = dot32(x, wd[...])
    decay = jnp.exp((jnp.minimum(pre, 0.0) - jnp.log1p(jnp.exp(-jnp.abs(pre)))) / 16.0)
    copies[3].wait()
    queries = dot32(x, wq[...]) * key_dim ** (-0.5)
    copies[4].wait()
    values = dot32(x, wv[...])
    columns = []
    for h in range(heads):
        part = slice(h * key_dim, (h + 1) * key_dim)
        pad = jnp.zeros((key_dim - 3 * rows, key_dim), F32)
        stacked = jnp.concatenate([keys[:, part], decay[:, part], queries[:, part], pad], axis=0)
        columns.append(stacked.T)
    for n in range(chunks):
        ins[n].wait()
        for b in range(n * chunk, (n + 1) * chunk):
            for h in range(heads):
                col = columns[h]
                v = values[b : b + 1, h * value_dim : (h + 1) * value_dim]
                new = (
                    col[:, rows + b : rows + b + 1] * state[b, h]
                    + col[:, b : b + 1] * v
                )
                fresh[b, h] = new
                readout[b : b + 1, h * value_dim : (h + 1) * value_dim] = jnp.sum(
                    col[:, 2 * rows + b : 2 * rows + b + 1] * new, axis=0, keepdims=True
                )
        outs[n].start()
    copies[5].wait()
    for h in range(heads):
        part = slice(h * value_dim, (h + 1) * value_dim)
        r = readout[:, part]
        scale = lax.rsqrt(jnp.mean(r * r, axis=-1, keepdims=True) + eps_norm)
        normed[:, part] = r * scale * gain[...]
    rounded = pltpu.make_async_copy(normed, normed_hbm, normed_sem.at[0])
    rounded.start()
    for one in outs:
        one.wait()
    rounded.wait()


def layer_kernel(
    n_ep,
    n_tp,
    cap,
    normed_hbm,
    wg_hbm,
    wo_hbm,
    tokens_hbm,
    norm_gain_hbm,
    norm_bias_hbm,
    group_w_hbm,
    router_w_hbm,
    routes_hbm,
    eg_hbm,
    eu_hbm,
    ed_hbm,
    out_ref,
    normed,
    wg,
    wo,
    tokens,
    norm_gain,
    norm_bias,
    group_w,
    router_w,
    routes,
    eg,
    eu,
    ed,
    part_mine,
    part_other,
    outgoing,
    arrived,
    results,
    returned,
    stat_mine,
    stat_other,
    in_sem,
    pair_sem,
    stat_sem,
    go_send,
    go_recv,
    back_send,
    back_recv,
):
    me = lax.axis_index("ep")
    core = lax.axis_index("tp")
    rows, width = tokens.shape
    half = width // n_tp
    per_group = router_w.shape[0] // group_w.shape[0]
    slots = n_ep * cap
    operands = [
        (tokens_hbm, tokens),
        (wg_hbm, wg),
        (normed_hbm, normed),
        (wo_hbm, wo),
        (routes_hbm, routes),
        (norm_gain_hbm, norm_gain),
        (norm_bias_hbm, norm_bias),
        (group_w_hbm, group_w),
        (router_w_hbm, router_w),
        (eg_hbm, eg),
        (eu_hbm, eu),
        (ed_hbm, ed),
    ]
    order = sorted(range(1, n_ep), key=lambda i: abs(2 * i - n_ep))

    def over_peers(body):
        if n_ep <= 32:
            for i in order:
                body(i)
        else:

            def step(i, carry):
                body(i)
                return carry

            lax.fori_loop(1, n_ep, step, 0)

    barrier = pltpu.get_barrier_semaphore()

    def greet(i):
        for c in range(n_tp):
            pl.semaphore_signal(
                barrier, inc=1, device_id=(lax.rem(me + i, n_ep), c), device_id_type=MESH
            )

    loads = [
        pltpu.make_async_copy(src, dst, in_sem.at[n]) for n, (src, dst) in enumerate(operands)
    ]
    for one in loads:
        one.start()
    over_peers(greet)
    for c in range(1, n_tp):
        pl.semaphore_signal(
            barrier, inc=1, device_id=(me, lax.rem(core + c, n_tp)), device_id_type=MESH
        )

    loads[0].wait()
    loads[1].wait()
    gate = dot32(tokens[...], wg[...])
    loads[2].wait()
    gated = (normed[...] * jax.nn.silu(gate)).astype(BF16)
    loads[3].wait()
    part_mine[...] = dot32(gated, wo[...]).astype(BF16)

    loads[4].wait()
    first, second = routes[0:1, :], routes[1:2, :]
    before = (
        lax.broadcasted_iota(jnp.int32, (rows, rows), 0)
        < lax.broadcasted_iota(jnp.int32, (rows, rows), 1)
    ).astype(BF16)

    def slot_of(count, to_expert):
        line = lax.broadcasted_iota(jnp.int32, (count, rows), 0)
        expert = to_expert(lax.div(line, cap))
        place = lax.rem(line, cap).astype(F32)
        hit0, hit1 = first == expert, second == expert
        either = jnp.where(hit0, 1.0, jnp.where(hit1, 1.0, 0.0))
        earlier = dot32(either.astype(BF16), before)
        placed = jnp.where(earlier == place, 1.0, 0.0)
        return jnp.where(hit0, placed, 0.0), jnp.where(hit1, placed, 0.0)

    send0, send1 = slot_of(slots, lambda j: j * n_tp + core)
    pick_send = (send0 + send1).astype(BF16)
    back0, back1 = slot_of(slots * n_tp, lambda j: j)
    for n in range(5, len(loads)):
        loads[n].wait()
    base = alpha_res * tokens[...].astype(F32) + part_mine[...].astype(F32)

    pl.semaphore_wait(barrier, n_ep * n_tp - 1)
    swap = pltpu.make_async_remote_copy(
        src_ref=part_mine,
        dst_ref=part_other,
        send_sem=pair_sem.at[0],
        recv_sem=pair_sem.at[1],
        device_id=(me, 1 - core),
        device_id_type=MESH,
    )
    swap.start()
    swap.wait()
    mixed = base + part_other[...].astype(F32)
    centered = mixed - jnp.mean(mixed, axis=-1, keepdims=True)
    spread = jnp.mean(centered * centered, axis=-1, keepdims=True)
    hidden = (
        centered * lax.rsqrt(spread + eps_norm) * norm_gain[0:1, :] + norm_bias[0:1, :]
    ).astype(BF16)

    outgoing[...] = dot32(pick_send, hidden).reshape(n_ep, cap, width).astype(BF16)

    def dispatch(i):
        there = lax.rem(me + i, n_ep)
        return pltpu.make_async_remote_copy(
            src_ref=outgoing.at[there],
            dst_ref=arrived.at[me],
            send_sem=go_send.at[i],
            recv_sem=go_recv.at[i],
            device_id=(there, core),
            device_id_type=MESH,
        )

    over_peers(lambda i: dispatch(i).start())
    arrived[me] = outgoing[me]

    across = (((1,), (1,)), ((), ()))
    group_logit = lax.dot_general(group_w[...], hidden, across, preferred_element_type=F32)
    expert_logit = lax.dot_general(router_w[...], hidden, across, preferred_element_type=F32)
    own_group = lax.div(first, per_group)
    group_hit = own_group == lax.broadcasted_iota(jnp.int32, group_logit.shape, 0)
    own_logit = jnp.sum(jnp.where(group_hit, group_logit, 0.0), axis=0, keepdims=True)
    share = 1.0 / jnp.sum(jnp.exp(group_logit - own_logit), axis=0, keepdims=True)
    expert_iota = lax.broadcasted_iota(jnp.int32, expert_logit.shape, 0)
    logit0 = jnp.sum(jnp.where(first == expert_iota, expert_logit, 0.0), axis=0, keepdims=True)
    logit1 = jnp.sum(jnp.where(second == expert_iota, expert_logit, 0.0), axis=0, keepdims=True)
    weighted = back0 * (share * jax.nn.sigmoid(logit0 - logit1)) + back1 * (
        share * jax.nn.sigmoid(logit1 - logit0)
    )
    upper = weighted.astype(BF16)
    lower = (weighted - upper.astype(F32)).astype(BF16)
    mine = jnp.where(core == 0, hidden[:, :half].astype(F32), hidden[:, half:].astype(F32))
    base = alpha_res * mine
    gain = jnp.where(core == 0, norm_gain[1:2, :half], norm_gain[1:2, half:])
    shift = jnp.where(core == 0, norm_bias[1:2, :half], norm_bias[1:2, half:])

    over_peers(lambda i: dispatch(i).wait())
    rows_in = arrived[...].astype(F32).reshape(slots, width).astype(BF16)
    gate_part = dot32(rows_in, eg[0])
    up_part = dot32(rows_in, eu[0])
    activation = (jax.nn.silu(gate_part) * up_part).astype(BF16)

    def send_back(i, c):
        there = lax.rem(me + i, n_ep)
        to = lax.rem(core + c, n_tp)
        return pltpu.make_async_remote_copy(
            src_ref=results.at[c, there],
            dst_ref=returned.at[me * n_tp + core],
            send_sem=back_send.at[c, i],
            recv_sem=back_recv.at[c, i],
            device_id=(there, to),
            device_id_type=MESH,
        )

    for c in range(n_tp):
        start = pl.multiple_of(lax.rem(core + c, n_tp) * half, half)
        result = dot32(activation, ed[0, :, pl.ds(start, half)])
        results[c] = result.reshape(n_ep, cap, half).astype(BF16)
        over_peers(lambda i: send_back(i, c).start())
        if c:
            send_back(0, c).start()
    returned[me * n_tp + core] = results[0, me]

    def home(i):
        for c in range(n_tp):
            send_back(i, c).wait()

    over_peers(home)
    for c in range(1, n_tp):
        send_back(0, c).wait()
    fetched = returned[...].astype(F32).reshape(slots * n_tp, half).astype(BF16)
    down = (((0,), (0,)), ((), ()))
    blended = (
        base
        + lax.dot_general(upper, fetched, down, preferred_element_type=F32)
        + lax.dot_general(lower, fetched, down, preferred_element_type=F32)
    )
    total = jnp.sum(blended, axis=1, keepdims=True)
    squares = jnp.sum(blended * blended, axis=1, keepdims=True)
    lane = lax.broadcasted_iota(jnp.int32, stat_mine.shape, 1)
    stats = jnp.where(lane == 0, total, squares)
    stat_mine[...] = stats
    trade = pltpu.make_async_remote_copy(
        src_ref=stat_mine,
        dst_ref=stat_other,
        send_sem=stat_sem.at[0],
        recv_sem=stat_sem.at[1],
        device_id=(me, 1 - core),
        device_id_type=MESH,
    )
    trade.start()
    trade.wait()
    both = stats + stat_other[...]
    row_mean = both[:, 0:1] / width
    spread = both[:, 1:2] / width - row_mean * row_mean
    out_ref[...] = (
        (blended - row_mean) * lax.rsqrt(spread + eps_norm) * gain + shift
    ).astype(BF16)


def on_device(
    n_ep,
    n_tp,
    tokens,
    recurrent_state,
    query_weight,
    key_weight,
    decay_weight,
    value_weight,
    gate_weight,
    head_gain,
    output_weight,
    norm_gain,
    norm_bias,
    group_router,
    router_weight,
    routes,
    expert_gate,
    expert_up,
    expert_down,
):
    rows, width = tokens.shape
    heads, key_dim, value_dim = recurrent_state.shape[1:]
    in_hbm = pl.BlockSpec(memory_space=pltpu.HBM)
    vmem = pl.BlockSpec(memory_space=pltpu.VMEM)
    chunk = 1
    chunks = rows // chunk
    dma = pltpu.SemaphoreType.DMA

    def like(a):
        return pltpu.VMEM(a.shape, a.dtype)

    gain_row = head_gain.reshape(1, value_dim)
    new_state, normed = pl.pallas_call(
        functools.partial(attention_kernel, chunk),
        out_shape=(
            jax.ShapeDtypeStruct(recurrent_state.shape, F32),
            jax.ShapeDtypeStruct((rows, heads * value_dim), F32),
        ),
        in_specs=[in_hbm] * 7,
        out_specs=(in_hbm, in_hbm),
        scratch_shapes=[
            like(tokens),
            like(recurrent_state),
            like(recurrent_state),
            like(query_weight),
            like(key_weight),
            like(decay_weight),
            like(value_weight),
            like(gain_row),
            pltpu.VMEM((rows, heads * value_dim), F32),
            pltpu.VMEM((rows, heads * value_dim), F32),
            dma((6,)),
            dma((chunks,)),
            dma((chunks,)),
            dma((1,)),
        ],
        compiler_params=pltpu.CompilerParams(vmem_limit_bytes=67043328),
        name="attention",
    )(
        tokens,
        recurrent_state,
        query_weight,
        key_weight,
        decay_weight,
        value_weight,
        gain_row,
    )
    experts = router_weight.shape[1]
    cap = 2 * max(1, rows // experts)
    half = width // n_tp
    operands = (
        normed,
        gate_weight,
        output_weight,
        tokens,
        norm_gain,
        norm_bias,
        group_router.T,
        router_weight.T,
        routes.T,
        expert_gate,
        expert_up,
        expert_down,
    )
    new_tokens = pl.pallas_call(
        functools.partial(layer_kernel, n_ep, n_tp, cap),
        out_shape=jax.ShapeDtypeStruct((rows, half), BF16),
        in_specs=[in_hbm] * len(operands),
        out_specs=vmem,
        scratch_shapes=[like(a) for a in operands]
        + [
            pltpu.VMEM((rows, width), BF16),
            pltpu.VMEM((rows, width), BF16),
            pltpu.VMEM((n_ep, cap, width), BF16),
            pltpu.VMEM((n_ep, cap, width), BF16),
            pltpu.VMEM((n_tp, n_ep, cap, half), BF16),
            pltpu.VMEM((n_ep * n_tp, cap, half), BF16),
            pltpu.VMEM((rows, 128), F32),
            pltpu.VMEM((rows, 128), F32),
            dma((len(operands),)),
            dma((2,)),
            dma((2,)),
            dma((n_ep,)),
            dma((n_ep,)),
            dma((n_tp, n_ep)),
            dma((n_tp, n_ep)),
        ],
        compiler_params=pltpu.CompilerParams(
            collective_id=0, has_side_effects=True, vmem_limit_bytes=67043328
        ),
        name="layer",
    )(*operands)
    return new_tokens, new_state


def solution(mesh):
    in_specs = (
        P("ep", None),
        P("ep", "tp", None, None),
        P(None, "tp"),
        P(None, "tp"),
        P(None, "tp"),
        P(None, "tp"),
        P(None, "tp"),
        P(),
        P("tp", None),
        P(),
        P(),
        P(),
        P(),
        P("ep", None),
        P(("ep", "tp"), None, None),
        P(("ep", "tp"), None, None),
        P(("ep", "tp"), None, None),
    )
    out_specs = (P("ep", "tp"), P("ep", "tp", None, None))
    return jax.shard_map(
        functools.partial(on_device, mesh.shape["ep"], mesh.shape["tp"]),
        mesh=mesh,
        in_specs=in_specs,
        out_specs=out_specs,
        check_vma=False,
    )
```

```python
import functools

import jax
import jax.numpy as jnp
from jax import lax
from jax.experimental import pallas as pl
from jax.experimental.pallas import tpu as pltpu
from jax.sharding import PartitionSpec as P

MESH = pl.DeviceIdType.MESH
alpha_res = 2.0**0.5
eps_norm = 1e-05
F32 = jnp.float32
BF16 = jnp.bfloat16


def dot32(a, b):
    return jnp.dot(a, b, preferred_element_type=F32)


def attention_kernel(
    chunk,
    tokens_hbm,
    state_hbm,
    wq_hbm,
    wk_hbm,
    wd_hbm,
    wv_hbm,
    wg_hbm,
    gain_hbm,
    new_hbm,
    gated_ref,
    tokens,
    state,
    fresh,
    wq,
    wk,
    wd,
    wv,
    wg,
    gain,
    readout,
    in_sem,
    state_sem,
    out_sem,
):
    rows, heads, key_dim, value_dim = state.shape
    chunks = rows // chunk
    small = [
        (tokens_hbm, tokens),
        (wk_hbm, wk),
        (wd_hbm, wd),
        (wq_hbm, wq),
        (wv_hbm, wv),
        (wg_hbm, wg),
        (gain_hbm, gain),
    ]
    copies = [
        pltpu.make_async_copy(src, dst, in_sem.at[n]) for n, (src, dst) in enumerate(small)
    ]
    ins = [
        pltpu.make_async_copy(
            state_hbm.at[pl.ds(n * chunk, chunk)], state.at[pl.ds(n * chunk, chunk)], state_sem.at[n]
        )
        for n in range(chunks)
    ]
    outs = [
        pltpu.make_async_copy(
            fresh.at[pl.ds(n * chunk, chunk)], new_hbm.at[pl.ds(n * chunk, chunk)], out_sem.at[n]
        )
        for n in range(chunks)
    ]
    for n in range(5):
        copies[n].start()
    for one in ins:
        one.start()
    copies[5].start()
    copies[6].start()

    copies[0].wait()
    x = tokens[...]
    copies[1].wait()
    keys = dot32(x, wk[...])
    copies[2].wait()
    pre = dot32(x, wd[...])
    decay = jnp.exp((jnp.minimum(pre, 0.0) - jnp.log1p(jnp.exp(-jnp.abs(pre)))) / 16.0)
    copies[3].wait()
    queries = dot32(x, wq[...]) * key_dim ** (-0.5)
    copies[4].wait()
    values = dot32(x, wv[...])
    columns = []
    for h in range(heads):
        part = slice(h * key_dim, (h + 1) * key_dim)
        pad = jnp.zeros((key_dim - 3 * rows, key_dim), F32)
        stacked = jnp.concatenate([keys[:, part], decay[:, part], queries[:, part], pad], axis=0)
        columns.append(stacked.T)
    for n in range(chunks):
        ins[n].wait()
        for b in range(n * chunk, (n + 1) * chunk):
            for h in range(heads):
                col = columns[h]
                v = values[b : b + 1, h * value_dim : (h + 1) * value_dim]
                new = (
                    col[:, rows + b : rows + b + 1] * state[b, h]
                    + col[:, b : b + 1] * v
                )
                fresh[b, h] = new
                readout[b : b + 1, h * value_dim : (h + 1) * value_dim] = jnp.sum(
                    col[:, 2 * rows + b : 2 * rows + b + 1] * new, axis=0, keepdims=True
                )
        outs[n].start()
    copies[5].wait()
    gate = dot32(x, wg[...])
    copies[6].wait()
    for h in range(heads):
        part = slice(h * value_dim, (h + 1) * value_dim)
        r = readout[:, part]
        scale = lax.rsqrt(jnp.mean(r * r, axis=-1, keepdims=True) + eps_norm)
        gated_ref[:, part] = (r * scale * gain[...] * jax.nn.silu(gate[:, part])).astype(BF16)
    for one in outs:
        one.wait()


def layer_kernel(
    n_ep,
    n_tp,
    cap,
    gated,
    wo_hbm,
    tokens_hbm,
    norm_gain_hbm,
    norm_bias_hbm,
    group_w_hbm,
    router_w_hbm,
    routes_hbm,
    eg_hbm,
    eu_hbm,
    ed_hbm,
    out_ref,
    wo,
    tokens,
    norm_gain,
    norm_bias,
    group_w,
    router_w,
    routes,
    eg,
    eu,
    ed,
    part_mine,
    part_other,
    outgoing,
    arrived,
    results,
    returned,
    stat_mine,
    stat_other,
    in_sem,
    pair_sem,
    stat_sem,
    go_send,
    go_recv,
    back_send,
    back_recv,
):
    me = lax.axis_index("ep")
    core = lax.axis_index("tp")
    rows, width = tokens.shape
    half = width // n_tp
    per_group = router_w.shape[0] // group_w.shape[0]
    slots = n_ep * cap
    operands = [
        (wo_hbm, wo),
        (routes_hbm, routes),
        (tokens_hbm, tokens),
        (norm_gain_hbm, norm_gain),
        (norm_bias_hbm, norm_bias),
        (group_w_hbm, group_w),
        (router_w_hbm, router_w),
        (eg_hbm, eg),
        (eu_hbm, eu),
        (ed_hbm, ed),
    ]
    order = sorted(range(1, n_ep), key=lambda i: abs(2 * i - n_ep))

    def over_peers(body):
        if n_ep <= 32:
            for i in order:
                body(i)
        else:

            def step(i, carry):
                body(i)
                return carry

            lax.fori_loop(1, n_ep, step, 0)

    barrier = pltpu.get_barrier_semaphore()

    def greet(i):
        for c in range(n_tp):
            pl.semaphore_signal(
                barrier, inc=1, device_id=(lax.rem(me + i, n_ep), c), device_id_type=MESH
            )

    loads = [
        pltpu.make_async_copy(src, dst, in_sem.at[n]) for n, (src, dst) in enumerate(operands)
    ]
    for one in loads:
        one.start()
    over_peers(greet)
    for c in range(1, n_tp):
        pl.semaphore_signal(
            barrier, inc=1, device_id=(me, lax.rem(core + c, n_tp)), device_id_type=MESH
        )

    loads[0].wait()
    part_mine[...] = dot32(gated[...], wo[...]).astype(BF16)

    loads[1].wait()
    first, second = routes[0:1, :], routes[1:2, :]
    before = (
        lax.broadcasted_iota(jnp.int32, (rows, rows), 0)
        < lax.broadcasted_iota(jnp.int32, (rows, rows), 1)
    ).astype(BF16)

    def slot_of(count, to_expert):
        line = lax.broadcasted_iota(jnp.int32, (count, rows), 0)
        expert = to_expert(lax.div(line, cap))
        place = lax.rem(line, cap).astype(F32)
        hit0, hit1 = first == expert, second == expert
        either = jnp.where(hit0, 1.0, jnp.where(hit1, 1.0, 0.0))
        earlier = dot32(either.astype(BF16), before)
        placed = jnp.where(earlier == place, 1.0, 0.0)
        return jnp.where(hit0, placed, 0.0), jnp.where(hit1, placed, 0.0)

    send0, send1 = slot_of(slots, lambda j: j * n_tp + core)
    pick_send = (send0 + send1).astype(BF16)
    back0, back1 = slot_of(slots * n_tp, lambda j: j)
    for n in range(2, len(loads)):
        loads[n].wait()
    base = alpha_res * tokens[...].astype(F32) + part_mine[...].astype(F32)

    pl.semaphore_wait(barrier, n_ep * n_tp - 1)
    swap = pltpu.make_async_remote_copy(
        src_ref=part_mine,
        dst_ref=part_other,
        send_sem=pair_sem.at[0],
        recv_sem=pair_sem.at[1],
        device_id=(me, 1 - core),
        device_id_type=MESH,
    )
    swap.start()
    swap.wait()
    mixed = base + part_other[...].astype(F32)
    centered = mixed - jnp.mean(mixed, axis=-1, keepdims=True)
    spread = jnp.mean(centered * centered, axis=-1, keepdims=True)
    hidden = (
        centered * lax.rsqrt(spread + eps_norm) * norm_gain[0:1, :] + norm_bias[0:1, :]
    ).astype(BF16)

    outgoing[...] = dot32(pick_send, hidden).reshape(n_ep, cap, width).astype(BF16)

    def dispatch(i):
        there = lax.rem(me + i, n_ep)
        return pltpu.make_async_remote_copy(
            src_ref=outgoing.at[there],
            dst_ref=arrived.at[me],
            send_sem=go_send.at[i],
            recv_sem=go_recv.at[i],
            device_id=(there, core),
            device_id_type=MESH,
        )

    over_peers(lambda i: dispatch(i).start())
    arrived[me] = outgoing[me]

    across = (((1,), (1,)), ((), ()))
    group_logit = lax.dot_general(group_w[...], hidden, across, preferred_element_type=F32)
    expert_logit = lax.dot_general(router_w[...], hidden, across, preferred_element_type=F32)
    own_group = lax.div(first, per_group)
    group_hit = own_group == lax.broadcasted_iota(jnp.int32, group_logit.shape, 0)
    own_logit = jnp.sum(jnp.where(group_hit, group_logit, 0.0), axis=0, keepdims=True)
    share = 1.0 / jnp.sum(jnp.exp(group_logit - own_logit), axis=0, keepdims=True)
    expert_iota = lax.broadcasted_iota(jnp.int32, expert_logit.shape, 0)
    logit0 = jnp.sum(jnp.where(first == expert_iota, expert_logit, 0.0), axis=0, keepdims=True)
    logit1 = jnp.sum(jnp.where(second == expert_iota, expert_logit, 0.0), axis=0, keepdims=True)
    weighted = back0 * (share * jax.nn.sigmoid(logit0 - logit1)) + back1 * (
        share * jax.nn.sigmoid(logit1 - logit0)
    )
    upper = weighted.astype(BF16)
    lower = (weighted - upper.astype(F32)).astype(BF16)
    mine = jnp.where(core == 0, hidden[:, :half].astype(F32), hidden[:, half:].astype(F32))
    base = alpha_res * mine
    gain = jnp.where(core == 0, norm_gain[1:2, :half], norm_gain[1:2, half:])
    shift = jnp.where(core == 0, norm_bias[1:2, :half], norm_bias[1:2, half:])

    over_peers(lambda i: dispatch(i).wait())
    rows_in = arrived[...].astype(F32).reshape(slots, width).astype(BF16)
    gate_part = dot32(rows_in, eg[0])
    up_part = dot32(rows_in, eu[0])
    activation = (jax.nn.silu(gate_part) * up_part).astype(BF16)

    def send_back(i, c):
        there = lax.rem(me + i, n_ep)
        to = lax.rem(core + c, n_tp)
        return pltpu.make_async_remote_copy(
            src_ref=results.at[c, there],
            dst_ref=returned.at[me * n_tp + core],
            send_sem=back_send.at[c, i],
            recv_sem=back_recv.at[c, i],
            device_id=(there, to),
            device_id_type=MESH,
        )

    for c in range(n_tp):
        start = pl.multiple_of(lax.rem(core + c, n_tp) * half, half)
        result = dot32(activation, ed[0, :, pl.ds(start, half)])
        results[c] = result.reshape(n_ep, cap, half).astype(BF16)
        over_peers(lambda i: send_back(i, c).start())
        if c:
            send_back(0, c).start()
    returned[me * n_tp + core] = results[0, me]

    def home(i):
        for c in range(n_tp):
            send_back(i, c).wait()

    over_peers(home)
    for c in range(1, n_tp):
        send_back(0, c).wait()
    fetched = returned[...].astype(F32).reshape(slots * n_tp, half).astype(BF16)
    down = (((0,), (0,)), ((), ()))
    blended = (
        base
        + lax.dot_general(upper, fetched, down, preferred_element_type=F32)
        + lax.dot_general(lower, fetched, down, preferred_element_type=F32)
    )
    total = jnp.sum(blended, axis=1, keepdims=True)
    squares = jnp.sum(blended * blended, axis=1, keepdims=True)
    lane = lax.broadcasted_iota(jnp.int32, stat_mine.shape, 1)
    stats = jnp.where(lane == 0, total, squares)
    stat_mine[...] = stats
    trade = pltpu.make_async_remote_copy(
        src_ref=stat_mine,
        dst_ref=stat_other,
        send_sem=stat_sem.at[0],
        recv_sem=stat_sem.at[1],
        device_id=(me, 1 - core),
        device_id_type=MESH,
    )
    trade.start()
    trade.wait()
    both = stats + stat_other[...]
    row_mean = both[:, 0:1] / width
    spread = both[:, 1:2] / width - row_mean * row_mean
    out_ref[...] = (
        (blended - row_mean) * lax.rsqrt(spread + eps_norm) * gain + shift
    ).astype(BF16)


def on_device(
    n_ep,
    n_tp,
    tokens,
    recurrent_state,
    query_weight,
    key_weight,
    decay_weight,
    value_weight,
    gate_weight,
    head_gain,
    output_weight,
    norm_gain,
    norm_bias,
    group_router,
    router_weight,
    routes,
    expert_gate,
    expert_up,
    expert_down,
):
    rows, width = tokens.shape
    heads, key_dim, value_dim = recurrent_state.shape[1:]
    in_hbm = pl.BlockSpec(memory_space=pltpu.HBM)
    vmem = pl.BlockSpec(memory_space=pltpu.VMEM)
    chunk = 4
    chunks = rows // chunk
    dma = pltpu.SemaphoreType.DMA

    def like(a):
        return pltpu.VMEM(a.shape, a.dtype)

    def pinned(arrays):
        return tuple(pltpu.with_memory_space_constraint(a, pltpu.HBM) for a in arrays)

    gain_row = head_gain.reshape(1, value_dim)
    new_state, gated = pl.pallas_call(
        functools.partial(attention_kernel, chunk),
        out_shape=(
            jax.ShapeDtypeStruct(recurrent_state.shape, F32),
            jax.ShapeDtypeStruct((rows, heads * value_dim), BF16),
        ),
        in_specs=[in_hbm] * 8,
        out_specs=(in_hbm, vmem),
        scratch_shapes=[
            like(tokens),
            like(recurrent_state),
            like(recurrent_state),
            like(query_weight),
            like(key_weight),
            like(decay_weight),
            like(value_weight),
            like(gate_weight),
            like(gain_row),
            pltpu.VMEM((rows, heads * value_dim), F32),
            dma((7,)),
            dma((chunks,)),
            dma((chunks,)),
        ],
        compiler_params=pltpu.CompilerParams(vmem_limit_bytes=40 * 1024 * 1024),
        name="attention",
    )(
        *pinned(
            (
                tokens,
                recurrent_state,
                query_weight,
                key_weight,
                decay_weight,
                value_weight,
                gate_weight,
                gain_row,
            )
        )
    )
    experts = router_weight.shape[1]
    cap = 2 * max(1, rows // experts)
    half = width // n_tp
    operands = (
        output_weight,
        tokens,
        norm_gain,
        norm_bias,
        group_router.T,
        router_weight.T,
        routes.T,
        expert_gate,
        expert_up,
        expert_down,
    )
    new_tokens = pl.pallas_call(
        functools.partial(layer_kernel, n_ep, n_tp, cap),
        out_shape=jax.ShapeDtypeStruct((rows, half), BF16),
        in_specs=[vmem] + [in_hbm] * len(operands),
        out_specs=vmem,
        scratch_shapes=[like(a) for a in operands]
        + [
            pltpu.VMEM((rows, width), BF16),
            pltpu.VMEM((rows, width), BF16),
            pltpu.VMEM((n_ep, cap, width), BF16),
            pltpu.VMEM((n_ep, cap, width), BF16),
            pltpu.VMEM((n_tp, n_ep, cap, half), BF16),
            pltpu.VMEM((n_ep * n_tp, cap, half), BF16),
            pltpu.VMEM((rows, 128), F32),
            pltpu.VMEM((rows, 128), F32),
            dma((len(operands),)),
            dma((2,)),
            dma((2,)),
            dma((n_ep,)),
            dma((n_ep,)),
            dma((n_tp, n_ep)),
            dma((n_tp, n_ep)),
        ],
        compiler_params=pltpu.CompilerParams(
            collective_id=0, has_side_effects=True, vmem_limit_bytes=40 * 1024 * 1024
        ),
        name="layer",
    )(gated, *pinned(operands))
    return new_tokens, new_state


def solution(mesh):
    in_specs = (
        P("ep", None),
        P("ep", "tp", None, None),
        P(None, "tp"),
        P(None, "tp"),
        P(None, "tp"),
        P(None, "tp"),
        P(None, "tp"),
        P(),
        P("tp", None),
        P(),
        P(),
        P(),
        P(),
        P("ep", None),
        P(("ep", "tp"), None, None),
        P(("ep", "tp"), None, None),
        P(("ep", "tp"), None, None),
    )
    out_specs = (P("ep", "tp"), P("ep", "tp", None, None))
    return jax.shard_map(
        functools.partial(on_device, mesh.shape["ep"], mesh.shape["tp"]),
        mesh=mesh,
        in_specs=in_specs,
        out_specs=out_specs,
        check_vma=False,
    )
```
